32 devices in a mesh: ep: 32 (over z, y, x, core).
Axes of the slice: x: 2, y: 2, z: 4, core: 2. Of those that a mesh axis runs over, the one named last changes fastest.
Arguments:
- tokens: bfloat16 [512, 1024], P('ep'), may hold values from -6 to 6
- lengths: int32 [512], P('ep'), may hold values from 1 to 8191
- cache_keys: bfloat16 [512, 128, 512], P('ep'), may hold values from -6 to 6
- cache_values: bfloat16 [512, 128, 1024], P('ep'), may hold values from -6 to 6
- retention_state: float32 [512, 4, 128, 256], P('ep'), may hold values from -24 to 24
- mix_gain: float32 [1024], replicated, may hold values from 0.1 to 1.9
- query_weight: bfloat16 [1024, 512], replicated, may hold values from -0.1875 to 0.1875
- key_weight: bfloat16 [1024, 512], replicated, may hold values from -0.1875 to 0.1875
- value_weight: bfloat16 [1024, 1024], replicated, may hold values from -0.1875 to 0.1875
- out_weight: bfloat16 [1024, 1024], replicated, may hold values from -0.1875 to 0.1875
- ffn_gain: float32 [1024], replicated, may hold values from 0.1 to 1.9
- routes: int32 [512, 6], P('ep'), may hold values from 0 to 31, all different within a row; in each aligned block of 16 rows (0 to 15, 16 to 31, ...) at most 8 rows name the same one
- route_scores: float32 [512, 6], P('ep'), may hold values from 0.05 to 1
- expert_gate: bfloat16 [32, 1024, 256], P('ep'), may hold values from -0.1875 to 0.1875
- expert_up: bfloat16 [32, 1024, 256], P('ep'), may hold values from -0.1875 to 0.1875
- expert_down: bfloat16 [32, 256, 1024], P('ep'), may hold values from -0.375 to 0.375
- shared_gate: bfloat16 [1024, 256], replicated, may hold values from -0.1875 to 0.1875
- shared_up: bfloat16 [1024, 256], replicated, may hold values from -0.1875 to 0.1875
- shared_down: bfloat16 [256, 1024], replicated, may hold values from -0.375 to 0.375
- dense_gate: bfloat16 [4096, 1024], P('ep'), may hold values from -0.1875 to 0.1875
- dense_up: bfloat16 [4096, 1024], P('ep'), may hold values from -0.1875 to 0.1875
- dense_down: bfloat16 [4096, 1024], P('ep'), may hold values from -0.09375 to 0.09375
- dense_mix: float32 [1024], replicated, may hold values from -3 to 3
Outputs:
- layer_out: bfloat16 [512, 1024], P('ep')
- new_keys: bfloat16 [512, 512], P('ep')
- new_values: bfloat16 [512, 1024], P('ep')
The draws below stay inside these ranges and needn't reach their ends.
Inputs may be any that keep to these rules, and one draw needn't show every extreme that they name: `routes`: each row names 6 different experts; among the rows of one device no expert is named more than 8 times.
All inputs are finite; a program needn't handle non-finite values.
Results may differ from the reference program's by a relative error of at most 0.012.
Values may be sent and summed in bfloat16 or wider, within the bound.
A program may use at most 128 MiB of HBM per device.

```python
import math
import jax
import jax.numpy as jnp
import numpy as np
from jax import lax

D = 1024
HEADS = 4
DK = 128
DV = 256
BLOCK = 128
SEQ_DEV = 16
SEQS = 512
EXPERTS = 32
TOP_K = 6
CAP = 8
EH = 256
SH = 256
DENSE_FF = 4096
N_EP = 32


def plant(values, stream_key, smallest, top_value):
    dims = values.shape
    spot = [jax.random.randint(jax.random.fold_in(stream_key, axis), (), 0, dims[axis]) for axis in range(len(dims))]
    values = values.at[tuple(spot)].set(smallest)
    longest = dims.index(max(dims))
    spot[longest] = (spot[longest] + 1) % dims[longest]
    return values.at[tuple(spot)].set(top_value)


def shard_levels(rng, dims, shards, low, high):
    factor_of = 1.0
    for axis_at, shards_of in shards:
        heights = jax.random.uniform(jax.random.fold_in(jax.random.fold_in(rng, 6), axis_at), (shards_of,), jnp.float32, low / len(shards), high / len(shards))
        factor_of = factor_of * jnp.repeat(jnp.exp(heights), dims[axis_at] // shards_of).reshape((-1,) + (1,) * (len(dims) - 1 - axis_at))
    return factor_of


def routed_block(key, own, number, rows, count, top, reach, slope):
    sequence = jax.random.permutation(key, count)
    crowded, common = portions_of(count, rows * top, reach, slope, True), portions_of(count, rows * top, reach, slope, False)
    places = jnp.arange(count)

    def named(tallies, offset_by):
        used = int((tallies > 0).sum())
        fixed = max(1, used // 4)
        passed = fixed + (places - fixed + offset_by * (used - fixed)) % max(1, count - fixed)
        return jnp.zeros((count,), jnp.int32).at[sequence[jnp.where(places < fixed, places, passed)]].set(jnp.asarray(tallies, jnp.int32))

    tallies = jnp.where(number % 4 == 0, named(crowded, number // 4), named(common, number - number // 4 - 1))
    mixed = jax.random.permutation(jax.random.fold_in(own, 3), count)
    donor, receiver = mixed[0:count // 2 * 2:2], mixed[1:count // 2 * 2:2]
    room = jnp.minimum(tallies[donor] - 1, reach - tallies[receiver]) // 2
    room = jnp.where((donor == sequence[0]) | (receiver == sequence[0]) | (tallies[receiver] == 0), 0, jnp.maximum(room, 0))
    passed = jax.random.randint(jax.random.fold_in(own, 4), (count // 2,), 0, 1 << 20) % (room + 1)
    tallies = tallies.at[donor].add(-passed).at[receiver].add(passed)
    members = jnp.searchsorted(jnp.cumsum(tallies), jnp.arange(rows * top), side="right").astype(jnp.int32)
    grid = members.reshape(top, rows).T
    grid = grid[jax.random.permutation(jax.random.fold_in(own, 1), rows)]
    offset_by = jax.random.randint(jax.random.fold_in(own, 2), (rows, 1), 0, top)
    return jnp.take_along_axis(grid, (jnp.arange(top)[None, :] + offset_by) % top, axis=1)


def portions_of(amount, total, limit, slope, full):
    portions = [(1 << 20) // math.isqrt(grade ** slope) + 1 for grade in range(1, amount + 1)]
    largest = limit if full else min(limit, max(-(-total // amount), total * portions[0] // sum(portions)))
    least = 1 if total - largest >= amount - 1 else 0
    counts, surplus = [largest] + [least] * (amount - 1), total - largest - least * (amount - 1)
    while surplus > 0:
        free = [i for i in range(1, amount) if counts[i] < largest] or [i for i in range(1, amount) if counts[i] < limit]
        pool, budget = sum([portions[i] for i in free]), surplus
        for i in free:
            addition = min(limit - counts[i], max(1, budget * portions[i] // pool), surplus)
            counts[i] = counts[i] + addition
            surplus = surplus - addition
    return np.array(counts)


def gaussian(own_key, dims, deviation, reach, shards=(), held_as=jnp.bfloat16):
    result = deviation * jax.random.normal(own_key, dims, jnp.float32)
    if shards:
        result = result * shard_levels(own_key, dims, shards, -0.22, 0.18)
    return jnp.clip(result, -reach, reach).astype(held_as)


def setup_inputs(seed: int = 0) -> dict:
    key_of = jax.random.split(jax.random.key(seed), 24)
    tokens = gaussian(key_of[0], (SEQS, D), 1.0, 6.0, ((0, 32),))
    lengths = plant(jax.random.randint(key_of[1], (SEQS,), 1, 8192), jax.random.fold_in(key_of[1], 1), 1, 8191).astype(jnp.int32)
    cache_keys = gaussian(key_of[2], (SEQS, BLOCK, HEADS * DK), 1.0, 6.0, ((0, 32),))
    cache_values = gaussian(key_of[3], (SEQS, BLOCK, HEADS * DV), 1.0, 6.0, ((0, 32),))
    retention_state = gaussian(key_of[4], (SEQS, HEADS, DK, DV), 4.0, 24.0, ((0, 32),), jnp.float32)
    mix_gain = jnp.clip(1.0 + 0.18 * jax.random.normal(key_of[5], (D,), jnp.float32), 0.1, 1.9)
    query_weight = gaussian(key_of[6], (D, HEADS * DK), D ** -0.5, 0.1875)
    key_weight = gaussian(key_of[7], (D, HEADS * DK), D ** -0.5, 0.1875)
    value_weight = gaussian(key_of[8], (D, HEADS * DV), D ** -0.5, 0.1875)
    out_weight = gaussian(key_of[9], (HEADS * DV, D), (HEADS * DV) ** -0.5, 0.1875)
    ffn_gain = jnp.clip(1.0 + 0.18 * jax.random.normal(key_of[10], (D,), jnp.float32), 0.1, 1.9)
    routes_keys = jax.random.split(jax.random.fold_in(key_of[11], 1), SEQS // SEQ_DEV)
    routes_turns = jax.random.permutation(jax.random.fold_in(key_of[11], 3), SEQS // SEQ_DEV)
    routes = jax.vmap(lambda own, number: routed_block(jax.random.fold_in(key_of[11], 2), own, number, SEQ_DEV, EXPERTS, TOP_K, CAP, 1))(routes_keys, routes_turns).reshape((SEQS, TOP_K))
    route_scores = jnp.clip(0.05 + 0.95 * jax.random.uniform(key_of[12], (SEQS, TOP_K), jnp.float32) ** shard_levels(key_of[12], (SEQS, TOP_K), ((0, 32),), -0.2, 0.2), 0.05, 1.0)
    expert_gate = gaussian(key_of[13], (EXPERTS, D, EH), D ** -0.5, 0.1875, ((0, 32),))
    expert_up = gaussian(key_of[14], (EXPERTS, D, EH), D ** -0.5, 0.1875, ((0, 32),))
    expert_down = gaussian(key_of[15], (EXPERTS, EH, D), EH ** -0.5, 0.375, ((0, 32),))
    shared_gate = gaussian(key_of[16], (D, SH), D ** -0.5, 0.1875)
    shared_up = gaussian(key_of[17], (D, SH), D ** -0.5, 0.1875)
    shared_down = gaussian(key_of[18], (SH, D), SH ** -0.5, 0.375)
    dense_gate = gaussian(key_of[19], (DENSE_FF, D), D ** -0.5, 0.1875, ((0, 32),))
    dense_up = gaussian(key_of[20], (DENSE_FF, D), D ** -0.5, 0.1875, ((0, 32),))
    dense_down = gaussian(key_of[21], (DENSE_FF, D), DENSE_FF ** -0.5, 0.09375, ((0, 32),))
    dense_mix = jnp.clip(jax.random.uniform(key_of[22], (D,), jnp.float32, -3.0, 3.0), -3.0, 3.0)
    return {"tokens": tokens, "lengths": lengths, "cache_keys": cache_keys, "cache_values": cache_values, "retention_state": retention_state, "mix_gain": mix_gain, "query_weight": query_weight, "key_weight": key_weight, "value_weight": value_weight, "out_weight": out_weight, "ffn_gain": ffn_gain, "routes": routes, "route_scores": route_scores, "expert_gate": expert_gate, "expert_up": expert_up, "expert_down": expert_down, "shared_gate": shared_gate, "shared_up": shared_up, "shared_down": shared_down, "dense_gate": dense_gate, "dense_up": dense_up, "dense_down": dense_down, "dense_mix": dense_mix}


eps = 1e-06
route_scale = 2.5
rope_base = 10000.0

def normed(values):
    return values * lax.rsqrt(lax.optimization_barrier(jnp.mean(values * values, axis=-1, keepdims=True)) + eps)

def log_decay(head_count):
    return jnp.log1p(-jnp.exp2(-5.0 - jnp.arange(head_count, dtype=jnp.float32)))

def rotate(values, positions):
    half_size = values.shape[-1] // 2
    inverse = rope_base ** (-jnp.arange(half_size, dtype=jnp.float32) / half_size)
    angles = positions.astype(jnp.float32)[:, None, None] * inverse[None, None, :]
    cosine = jnp.cos(angles)
    sine_part = jnp.sin(angles)
    first_half = values[..., :half_size]
    second = values[..., half_size:]
    return jnp.concatenate([first_half * cosine - second * sine_part, first_half * sine_part + second * cosine], axis=-1)

def swiglu(inputs, w_gate, w_up, w_down):
    gate_part = jnp.dot(inputs, w_gate, preferred_element_type=jnp.float32)
    up_part = jnp.dot(inputs, w_up, preferred_element_type=jnp.float32)
    hidden = (jax.nn.silu(gate_part) * up_part).astype(jnp.bfloat16)
    return jnp.dot(hidden, w_down, preferred_element_type=jnp.float32)

def retain(tokens, lengths, mix_gain, w_query, w_key, w_value, w_out, cache_keys, cache_values, carry_state):
    seq_count, head_count, key_size, value_size = carry_state.shape
    block_size = cache_keys.shape[1]
    widened = tokens.astype(jnp.float32)
    normal_in = (normed(widened) * mix_gain).astype(jnp.bfloat16)
    raw_query = jnp.dot(normal_in, w_query, preferred_element_type=jnp.float32).reshape(seq_count, head_count, key_size)
    raw_key = jnp.dot(normal_in, w_key, preferred_element_type=jnp.float32).reshape(seq_count, head_count, key_size)
    raw_value = jnp.dot(normal_in, w_value, preferred_element_type=jnp.float32).reshape(seq_count, head_count, value_size)
    queries = (rotate(raw_query, lengths) * key_size ** (-0.5)).astype(jnp.bfloat16)
    new_keys = rotate(raw_key, lengths).astype(jnp.bfloat16)
    new_values = raw_value.astype(jnp.bfloat16)
    filled = lengths % block_size
    decay_rate = log_decay(head_count)
    places = jnp.arange(block_size, dtype=jnp.int32)
    stored_keys = cache_keys.reshape(seq_count, block_size, head_count, key_size)
    stored_values = cache_values.reshape(seq_count, block_size, head_count, value_size)
    scores = jnp.einsum('shd,sjhd->shj', queries.astype(jnp.float32), stored_keys.astype(jnp.float32))
    distance = jnp.maximum(filled[:, None] - places[None, :], 0).astype(jnp.float32)
    live_mask = places[None, :] < filled[:, None]
    weighted = jnp.where(live_mask[:, None, :], scores * jnp.exp(distance[:, None, :] * decay_rate[None, :, None]), 0.0).astype(jnp.bfloat16)
    own_weight = lax.optimization_barrier(jnp.sum(queries.astype(jnp.float32) * new_keys.astype(jnp.float32), axis=-1)).astype(jnp.bfloat16)
    inside = jnp.einsum('shj,sjhe->she', weighted.astype(jnp.float32), stored_values.astype(jnp.float32))
    inside = inside + own_weight.astype(jnp.float32)[:, :, None] * new_values.astype(jnp.float32)
    carried = jnp.einsum('shd,shde->she', queries.astype(jnp.float32), carry_state, precision=lax.Precision.HIGHEST)
    carried = carried * jnp.exp((filled.astype(jnp.float32)[:, None] + 1.0) * decay_rate[None, :])[:, :, None]
    headed = normed(inside + carried).astype(jnp.bfloat16).reshape(seq_count, head_count * value_size)
    mixer_out = jnp.dot(headed, w_out, preferred_element_type=jnp.float32)
    residual = widened + normed(mixer_out)
    return (residual, new_keys.reshape(seq_count, head_count * key_size), new_values.reshape(seq_count, head_count * value_size))

def reference(tokens, lengths, cache_keys, cache_values, retention_state, mix_gain, query_weight, key_weight, value_weight, out_weight, ffn_gain, routes, route_scores, expert_gate, expert_up, expert_down, shared_gate, shared_up, shared_down, dense_gate, dense_up, dense_down, dense_mix):
    residual, new_keys, new_values = retain(tokens, lengths, mix_gain, query_weight, key_weight, value_weight, out_weight, cache_keys, cache_values, retention_state)
    normal_ffn = (normed(residual) * ffn_gain).astype(jnp.bfloat16)
    shared_out = swiglu(normal_ffn, shared_gate, shared_up, shared_down)
    dense_gate_part = jnp.dot(normal_ffn, dense_gate.T, preferred_element_type=jnp.float32)
    dense_up_part = jnp.dot(normal_ffn, dense_up.T, preferred_element_type=jnp.float32)
    dense_hidden = (jax.nn.silu(dense_gate_part) * dense_up_part).astype(jnp.bfloat16)
    dense_out = jnp.dot(dense_hidden, dense_down, preferred_element_type=jnp.float32)
    route_weight = route_scores / lax.optimization_barrier(jnp.sum(route_scores, axis=-1, keepdims=True)) * route_scale
    flat_routes = routes.reshape(-1)
    flat_weight = route_weight.reshape(-1)
    most_rows = N_EP * CAP
    slot_rank = jnp.arange(most_rows, dtype=jnp.int32)

    def one_expert(running, expert_id):
        hits = flat_routes == expert_id
        hit_count = jnp.sum(hits.astype(jnp.int32))
        picked = jnp.nonzero(hits, size=most_rows, fill_value=0)[0].astype(jnp.int32)
        is_valid = slot_rank < hit_count
        row_ids = picked // TOP_K
        outputs = swiglu(normal_ffn[row_ids], expert_gate[expert_id], expert_up[expert_id], expert_down[expert_id]).astype(jnp.bfloat16)
        added = jnp.where(is_valid[:, None], outputs.astype(jnp.float32) * flat_weight[picked][:, None], 0.0)
        return (running.at[row_ids].add(added), None)
    routed, _ = lax.scan(one_expert, jnp.zeros(residual.shape, jnp.float32), jnp.arange(EXPERTS, dtype=jnp.int32))
    combined = shared_out + routed + jax.nn.sigmoid(dense_mix) * dense_out
    layer_out = (residual + normed(combined)).astype(jnp.bfloat16)
    return (layer_out, new_keys, new_values)
```

```python
import functools
import math

import jax
import jax.numpy as jnp
from jax import lax
from jax.experimental import pallas as pl
from jax.experimental.pallas import tpu as pltpu
from jax.sharding import PartitionSpec as P

eps = 1e-06
route_scale = 2.5
rope_base = 10000.0


def normed(values):
    return values * lax.rsqrt(jnp.mean(values * values, axis=-1, keepdims=True) + eps)


def log_decay(head_count):
    return jnp.log1p(-jnp.exp2(-5.0 - jnp.arange(head_count, dtype=jnp.float32)))


def rotate(values, positions):
    half_size = values.shape[-1] // 2
    inverse = rope_base ** (-jnp.arange(half_size, dtype=jnp.float32) / half_size)
    angles = positions.astype(jnp.float32)[:, None, None] * inverse[None, None, :]
    cosine = jnp.cos(angles)
    sine_part = jnp.sin(angles)
    first_half = values[..., :half_size]
    second = values[..., half_size:]
    return jnp.concatenate(
        [first_half * cosine - second * sine_part, first_half * sine_part + second * cosine],
        axis=-1,
    )


def retain(
    tokens, lengths, mix_gain, w_query, w_key, w_value, w_out, cache_keys, cache_values, carry_state
):
    seq_count, head_count, key_size, value_size = carry_state.shape
    block_size = cache_keys.shape[1]
    widened = tokens.astype(jnp.float32)
    normal_in = (normed(widened) * mix_gain).astype(jnp.bfloat16)
    raw_query = jnp.dot(normal_in, w_query, preferred_element_type=jnp.float32).reshape(
        seq_count, head_count, key_size
    )
    raw_key = jnp.dot(normal_in, w_key, preferred_element_type=jnp.float32).reshape(
        seq_count, head_count, key_size
    )
    raw_value = jnp.dot(normal_in, w_value, preferred_element_type=jnp.float32).reshape(
        seq_count, head_count, value_size
    )
    queries = (rotate(raw_query, lengths) * key_size ** (-0.5)).astype(jnp.bfloat16)
    new_keys = rotate(raw_key, lengths).astype(jnp.bfloat16)
    new_values = raw_value.astype(jnp.bfloat16)
    filled = lengths % block_size
    decay_rate = log_decay(head_count)
    places = jnp.arange(block_size, dtype=jnp.int32)
    stored_keys = cache_keys.reshape(seq_count, block_size, head_count, key_size)
    stored_values = cache_values.reshape(seq_count, block_size, head_count, value_size)
    scores = jnp.einsum("shd,sjhd->shj", queries, stored_keys, preferred_element_type=jnp.float32)
    distance = jnp.maximum(filled[:, None] - places[None, :], 0).astype(jnp.float32)
    live_mask = places[None, :] < filled[:, None]
    weighted = jnp.where(
        live_mask[:, None, :],
        scores * jnp.exp(distance[:, None, :] * decay_rate[None, :, None]),
        0.0,
    ).astype(jnp.bfloat16)
    own_weight = jnp.sum(
        queries.astype(jnp.float32) * new_keys.astype(jnp.float32), axis=-1
    ).astype(jnp.bfloat16)
    inside = jnp.einsum(
        "shj,sjhe->she", weighted, stored_values, preferred_element_type=jnp.float32
    )
    inside = inside + own_weight.astype(jnp.float32)[:, :, None] * new_values.astype(jnp.float32)
    carried = jnp.einsum(
        "shd,shde->she", queries.astype(jnp.float32), carry_state, precision=lax.Precision.HIGHEST
    )
    carried = (
        carried
        * jnp.exp((filled.astype(jnp.float32)[:, None] + 1.0) * decay_rate[None, :])[:, :, None]
    )
    headed = (
        normed(inside + carried).astype(jnp.bfloat16).reshape(seq_count, head_count * value_size)
    )
    mixer_out = jnp.dot(headed, w_out, preferred_element_type=jnp.float32)
    residual = widened + normed(mixer_out)
    return (
        residual,
        new_keys.reshape(seq_count, head_count * key_size),
        new_values.reshape(seq_count, head_count * value_size),
    )


f32 = jnp.float32
bf16 = jnp.bfloat16


def slice_dims(device_count):
    side = max(1, math.isqrt(device_count // 8))
    return device_count // (2 * side * side), side, side


def mm(a, b):
    return lax.dot_general(a, b, (((1,), (0,)), ((), ())), preferred_element_type=f32)


def mm_t(a, b):
    return lax.dot_general(a, b, (((1,), (1,)), ((), ())), preferred_element_type=f32)


def silu(v):
    return v / (1.0 + jnp.exp(-v))


def channel_mixer(
    dims,
    width,
    expert_count,
    block_ref,
    residual_ref,
    mix_ref,
    eg_hbm,
    eu_hbm,
    ed_hbm,
    dg_hbm,
    du_hbm,
    dd_hbm,
    sg_hbm,
    su_hbm,
    sd_hbm,
    out_ref,
    eg,
    eu,
    ed,
    dg,
    du,
    dd,
    sg,
    su,
    sd,
    gathered,
    partial,
    in_core,
    sum_core,
    in2a,
    in2b,
    sum2a,
    sum2b,
    in3a,
    in3b,
    sum3,
    in4,
    total,
    w_sem,
    own_sem,
    gz_s,
    gz_r,
    g2a_s,
    g2a_r,
    g2b_s,
    g2b_r,
    g3a_s,
    g3a_r,
    g3b_s,
    g3b_r,
    g4_s,
    g4_r,
    r1_s,
    r1_r,
    r2a_s,
    r2a_r,
    r2b_s,
    r2b_r,
    r3a_s,
    r3a_r,
    r3b_s,
    r3b_r,
    r4_s,
    r4_r,
):
    zs, ys, xs = dims
    half = width // 2
    me = lax.axis_index("ep")
    core = lax.rem(me, 2)
    x = lax.rem(me // 2, xs)
    y = lax.rem(me // (2 * xs), ys)
    z = me // (2 * xs * ys)
    other = 1 - core

    def turn(at, by, size):
        return lax.rem(at + by + size, size)

    def device(zz, yy, xx, cc):
        return ((zz * ys + yy) * xs + xx) * 2 + cc

    def z_peer(by):
        return device(turn(z, by, zs), y, x, core)

    def y_peer(by):
        return device(z, turn(y, by, ys), x, core)

    def x_peer(by):
        return device(z, y, turn(x, by, xs), core)

    mate = device(z, y, x, other)
    peers = (
        [z_peer(p) for p in range(1, zs)]
        + [y_peer(p) for p in range(1, ys)]
        + [x_peer(p) for p in range(1, xs)]
        + [mate]
    )

    loads = []
    for at, (a, b) in enumerate(
        [
            (sg_hbm, sg),
            (su_hbm, su),
            (sd_hbm, sd),
            (eg_hbm.at[0], eg),
            (eu_hbm.at[0], eu),
            (ed_hbm.at[0], ed),
            (dg_hbm, dg),
            (du_hbm, du),
            (dd_hbm, dd),
        ]
    ):
        load = pltpu.make_async_copy(a, b, w_sem.at[at])
        load.start()
        loads.append(load)
    own = pltpu.make_async_copy(block_ref, gathered.at[z, y, x, core], own_sem)
    own.start()

    barrier = pltpu.get_barrier_semaphore()
    for peer in peers:
        pl.semaphore_signal(
            barrier, inc=1, device_id=(peer,), device_id_type=pl.DeviceIdType.MESH
        )
    pl.semaphore_wait(barrier, len(peers))

    started = []

    def send(source, target, send_sem, recv_sem, peer):
        copy = pltpu.make_async_remote_copy(
            src_ref=source,
            dst_ref=target,
            send_sem=send_sem,
            recv_sem=recv_sem,
            device_id=(peer,),
            device_id_type=pl.DeviceIdType.MESH,
        )
        copy.start()
        started.append(copy)
        return copy

    own.wait()
    for_z, for2, for3, for4 = {}, {}, {}, {}
    for o in range(1, zs):
        mine = gathered.at[z, y, x, core]
        for_z[o] = send(mine, mine, gz_s.at[o - 1], gz_r.at[o - 1], z_peer(o))

    def spread2(o):
        at = turn(z, -o, zs)
        if o:
            for_z[o].wait_recv()
        a = gathered.at[at, y, x, core, :, pl.ds(0, half)]
        b = gathered.at[at, y, x, core, :, pl.ds(half, gathered.shape[-1] - half)]
        for2[o] = [
            send(a, a, g2a_s.at[o, p - 1], g2a_r.at[o, p - 1], y_peer(p)) for p in range(1, ys)
        ] + [send(b, b, g2b_s.at[o, p - 1], g2b_r.at[o, p - 1], x_peer(p)) for p in range(1, xs)]

    def spread3(o):
        at = turn(z, -o, zs)
        for copy in for2[o]:
            copy.wait_recv()
        a = gathered.at[at, :, x, core, :, pl.ds(0, half)]
        b = gathered.at[at, y, :, core, :, pl.ds(half, gathered.shape[-1] - half)]
        for3[o] = [
            send(a, a, g3a_s.at[o, p - 1], g3a_r.at[o, p - 1], x_peer(p)) for p in range(1, xs)
        ] + [send(b, b, g3b_s.at[o, p - 1], g3b_r.at[o, p - 1], y_peer(p)) for p in range(1, ys)]

    def spread4(o):
        at = turn(z, -o, zs)
        for copy in for3[o]:
            copy.wait_recv()
        a = gathered.at[at, :, :, core]
        for4[o] = send(a, a, g4_s.at[o], g4_r.at[o], mate)

    to1, to2, to3, to4 = {}, {}, {}, {}
    gate = 1.0 / (1.0 + jnp.exp(-mix_ref[...]))

    def branches(o):
        at = turn(z, -o, zs)
        if o == 0:
            for load in loads[3:]:
                load.wait()
        for4[o].wait_recv()
        rows = ys * xs * 2 * gathered.shape[4]
        block = gathered[at].reshape(rows, gathered.shape[-1])
        inputs = block[:, :width]
        extra = block[:, width:].astype(f32)
        lane = lax.broadcasted_iota(jnp.int32, extra.shape, 1)
        chosen = (lane == me) | (lane == me + expert_count)
        weight = jnp.sum(jnp.where(chosen, extra, 0.0), axis=1, keepdims=True)
        hidden = (silu(mm(inputs, eg[...])) * mm(inputs, eu[...])).astype(bf16)
        dense = (silu(mm_t(inputs, dg[...])) * mm_t(inputs, du[...])).astype(bf16)
        terms = weight * mm(hidden, ed[...]) + gate * mm(dense, dd[...])
        partial[at] = terms.astype(bf16).reshape(partial.shape[1:])
        to1[o] = send(
            partial.at[at, :, :, other], in_core.at[o], r1_s.at[o], r1_r.at[o], mate
        )

    def reduce2(o):
        at = turn(z, -o, zs)
        to1[o].wait_recv()
        sum_core[o] = (partial[at, :, :, core].astype(f32) + in_core[o].astype(f32)).astype(bf16)
        to2[o] = [
            send(
                sum_core.at[o, :, turn(x, p, xs), :, pl.ds(0, half)],
                in2a.at[o, p - 1],
                r2a_s.at[o, p - 1],
                r2a_r.at[o, p - 1],
                x_peer(p),
            )
            for p in range(1, xs)
        ] + [
            send(
                sum_core.at[o, turn(y, p, ys), :, :, pl.ds(half, width - half)],
                in2b.at[o, p - 1],
                r2b_s.at[o, p - 1],
                r2b_r.at[o, p - 1],
                y_peer(p),
            )
            for p in range(1, ys)
        ]

    def reduce3(o):
        for copy in to2[o]:
            copy.wait_recv()
        a = sum_core[o, :, x, :, 0:half].astype(f32)
        for p in range(1, xs):
            a = a + in2a[o, p - 1].astype(f32)
        sum2a[o] = a.astype(bf16)
        b = sum_core[o, y, :, :, half:width].astype(f32)
        for p in range(1, ys):
            b = b + in2b[o, p - 1].astype(f32)
        sum2b[o] = b.astype(bf16)
        to3[o] = [
            send(
                sum2a.at[o, turn(y, p, ys)],
                in3a.at[o, p - 1],
                r3a_s.at[o, p - 1],
                r3a_r.at[o, p - 1],
                y_peer(p),
            )
            for p in range(1, ys)
        ] + [
            send(
                sum2b.at[o, turn(x, p, xs)],
                in3b.at[o, p - 1],
                r3b_s.at[o, p - 1],
                r3b_r.at[o, p - 1],
                x_peer(p),
            )
            for p in range(1, xs)
        ]

    def reduce4(o):
        for copy in to3[o]:
            copy.wait_recv()
        a = sum2a[o, y].astype(f32)
        for p in range(1, ys):
            a = a + in3a[o, p - 1].astype(f32)
        b = sum2b[o, x].astype(f32)
        for p in range(1, xs):
            b = b + in3b[o, p - 1].astype(f32)
        if o == 0:
            total[:, 0:half] = total[:, 0:half] + a
            total[:, half:width] = total[:, half:width] + b
        else:
            sum3[o - 1, :, 0:half] = a.astype(bf16)
            sum3[o - 1, :, half:width] = b.astype(bf16)
            to4[o] = send(
                sum3.at[o - 1], in4.at[o - 1], r4_s.at[o - 1], r4_r.at[o - 1], z_peer(-o)
            )

    def shared():
        for load in loads[:3]:
            load.wait()
        inputs = block_ref[:, :width]
        hidden = (silu(mm(inputs, sg[...])) * mm(inputs, su[...])).astype(bf16)
        total[...] = mm(hidden, sd[...])

    stages = [spread2, spread3, spread4, branches, reduce2, reduce3, reduce4]
    for step in range(zs + len(stages) - 1):
        for at, stage in enumerate(stages):
            if 0 <= step - at < zs:
                stage(step - at)
        if step == 0:
            shared()

    combined = total[...]
    for o in range(1, zs):
        to4[o].wait_recv()
        combined = combined + in4[o - 1].astype(f32)
    scale = lax.rsqrt(jnp.mean(combined * combined, axis=-1, keepdims=True) + eps)
    out_ref[...] = (residual_ref[...] + combined * scale).astype(bf16)
    for copy in started:
        copy.wait_send()


def mixed_channels(block, residual, dense_mix, weights, expert_count, device_count):
    seq_count, width = residual.shape
    wide = block.shape[1]
    zs, ys, xs = slice_dims(device_count)
    half = width // 2
    rest = width - half
    y1, x1, z1 = max(ys - 1, 1), max(xs - 1, 1), max(zs - 1, 1)
    held = [pltpu.VMEM(w.shape[-2:], bf16) for w in weights]
    dma = pltpu.SemaphoreType.DMA
    buffers = [
        pltpu.VMEM((zs, ys, xs, 2, seq_count, wide), bf16),
        pltpu.VMEM((zs, ys, xs, 2, seq_count, width), bf16),
        pltpu.VMEM((zs, ys, xs, seq_count, width), bf16),
        pltpu.VMEM((zs, ys, xs, seq_count, width), bf16),
        pltpu.VMEM((zs, x1, ys, seq_count, half), bf16),
        pltpu.VMEM((zs, y1, xs, seq_count, rest), bf16),
        pltpu.VMEM((zs, ys, seq_count, half), bf16),
        pltpu.VMEM((zs, xs, seq_count, rest), bf16),
        pltpu.VMEM((zs, y1, seq_count, half), bf16),
        pltpu.VMEM((zs, x1, seq_count, rest), bf16),
        pltpu.VMEM((z1, seq_count, width), bf16),
        pltpu.VMEM((z1, seq_count, width), bf16),
        pltpu.VMEM((seq_count, width), f32),
    ]
    sems = [dma((len(weights),)), dma]
    for shape in [
        (z1,),
        (zs, y1),
        (zs, x1),
        (zs, x1),
        (zs, y1),
        (zs,),
        (zs,),
        (zs, x1),
        (zs, y1),
        (zs, y1),
        (zs, x1),
        (z1,),
    ]:
        sems += [dma(shape), dma(shape)]
    vmem = pl.BlockSpec(memory_space=pltpu.VMEM)
    return pl.pallas_call(
        functools.partial(channel_mixer, (zs, ys, xs), width, expert_count),
        out_shape=jax.ShapeDtypeStruct((seq_count, width), bf16),
        in_specs=[vmem] * 3 + [pl.BlockSpec(memory_space=pl.ANY)] * len(weights),
        out_specs=vmem,
        scratch_shapes=held + buffers + sems,
        compiler_params=pltpu.CompilerParams(
            collective_id=0, has_side_effects=True, vmem_limit_bytes=56 * 1024 * 1024
        ),
    )(block, residual, dense_mix.reshape(1, width), *weights)


def per_device(
    tokens,
    lengths,
    cache_keys,
    cache_values,
    retention_state,
    mix_gain,
    query_weight,
    key_weight,
    value_weight,
    out_weight,
    ffn_gain,
    routes,
    route_scores,
    expert_gate,
    expert_up,
    expert_down,
    shared_gate,
    shared_up,
    shared_down,
    dense_gate,
    dense_up,
    dense_down,
    dense_mix,
):
    residual, new_keys, new_values = retain(
        tokens,
        lengths,
        mix_gain,
        query_weight,
        key_weight,
        value_weight,
        out_weight,
        cache_keys,
        cache_values,
        retention_state,
    )
    normal_ffn = (normed(residual) * ffn_gain).astype(jnp.bfloat16)
    device_count = lax.axis_size("ep")
    expert_count = device_count * expert_gate.shape[0]
    route_weight = route_scores / jnp.sum(route_scores, axis=-1, keepdims=True) * route_scale
    named = routes[:, :, None] == jnp.arange(expert_count, dtype=jnp.int32)[None, None, :]
    by_expert = jnp.sum(jnp.where(named, route_weight[:, :, None], 0.0), axis=1)
    upper = lax.reduce_precision(by_expert, 8, 7)
    pad = -(2 * expert_count) % 128
    block = jnp.concatenate(
        [
            normal_ffn,
            upper.astype(bf16),
            (by_expert - upper).astype(bf16),
            jnp.zeros((routes.shape[0], pad), bf16),
        ],
        axis=1,
    )
    weights = (
        expert_gate,
        expert_up,
        expert_down,
        dense_gate,
        dense_up,
        dense_down,
        shared_gate,
        shared_up,
        shared_down,
    )
    layer_out = mixed_channels(block, residual, dense_mix, weights, expert_count, device_count)
    return (layer_out, new_keys, new_values)


def solution(mesh):
    in_specs = (
        P("ep", None),
        P("ep"),
        P("ep", None, None),
        P("ep", None, None),
        P("ep", None, None, None),
        P(),
        P(),
        P(),
        P(),
        P(),
        P(),
        P("ep", None),
        P("ep", None),
        P("ep", None, None),
        P("ep", None, None),
        P("ep", None, None),
        P(),
        P(),
        P(),
        P("ep", None),
        P("ep", None),
        P("ep", None),
        P(),
    )
    out_specs = (P("ep", None), P("ep", None), P("ep", None))
    return jax.shard_map(
        per_device, mesh=mesh, in_specs=in_specs, out_specs=out_specs, check_vma=False
    )
```

```python
import functools
import math

import jax
import jax.numpy as jnp
from jax import lax
from jax.experimental import pallas as pl
from jax.experimental.pallas import tpu as pltpu
from jax.sharding import PartitionSpec as P

eps = 1e-06
route_scale = 2.5
rope_base = 10000.0


def normed(values):
    return values * lax.rsqrt(jnp.mean(values * values, axis=-1, keepdims=True) + eps)


def log_decay(head_count):
    return jnp.log1p(-jnp.exp2(-5.0 - jnp.arange(head_count, dtype=jnp.float32)))


def rotate(values, positions):
    half_size = values.shape[-1] // 2
    inverse = rope_base ** (-jnp.arange(half_size, dtype=jnp.float32) / half_size)
    angles = positions.astype(jnp.float32)[:, None, None] * inverse[None, None, :]
    cosine = jnp.cos(angles)
    sine_part = jnp.sin(angles)
    first_half = values[..., :half_size]
    second = values[..., half_size:]
    return jnp.concatenate(
        [first_half * cosine - second * sine_part, first_half * sine_part + second * cosine],
        axis=-1,
    )


f32 = jnp.float32
bf16 = jnp.bfloat16


def slice_dims(device_count):
    side = max(1, math.isqrt(device_count // 8))
    return device_count // (2 * side * side), side, side


def mm(a, b):
    return lax.dot_general(a, b, (((1,), (0,)), ((), ())), preferred_element_type=f32)


def mm_t(a, b):
    return lax.dot_general(a, b, (((1,), (1,)), ((), ())), preferred_element_type=f32)


def block_reads(query_ref, column_ref, decay_ref, key_ref, value_ref, state_ref, out_ref):
    head_count, value_size = state_ref.shape[1], state_ref.shape[3]
    for at in range(key_ref.shape[0]):
        scores = mm_t(query_ref[at], key_ref[at])
        cross = mm((scores * decay_ref[at]).astype(bf16), value_ref[at])
        row = lax.broadcasted_iota(jnp.int32, cross.shape, 0) * value_size
        lane = lax.broadcasted_iota(jnp.int32, cross.shape, 1)
        own_head = (lane >= row) & (lane < row + value_size)
        inside = jnp.sum(jnp.where(own_head, cross, 0.0), axis=0, keepdims=True)
        columns = column_ref[at]
        carried = [
            jnp.sum(columns[:, h : h + 1] * state_ref[at, h], axis=0, keepdims=True)
            for h in range(head_count)
        ]
        out_ref[at] = inside + jnp.concatenate(carried, axis=1)


def read_blocks(spread, columns, decay, cache_keys, cache_values, carry_state):
    operands = (spread, columns, decay, cache_keys, cache_values, carry_state)
    seq_count, width = cache_values.shape[0], cache_values.shape[2]
    step = 2 if seq_count % 2 == 0 else 1

    def rows(shape):
        return pl.BlockSpec((step,) + shape[1:], lambda i: (i,) + (0,) * (len(shape) - 1))

    return pl.pallas_call(
        block_reads,
        grid=(seq_count // step,),
        out_shape=jax.ShapeDtypeStruct((seq_count, 1, width), f32),
        in_specs=[rows(a.shape) for a in operands],
        out_specs=rows((seq_count, 1, width)),
    )(*operands)


def retain(
    tokens, lengths, mix_gain, w_query, w_key, w_value, w_out, cache_keys, cache_values, carry_state
):
    seq_count, head_count, key_size, value_size = carry_state.shape
    block_size = cache_keys.shape[1]
    widened = tokens.astype(jnp.float32)
    normal_in = (normed(widened) * mix_gain).astype(jnp.bfloat16)
    raw_query = jnp.dot(normal_in, w_query, preferred_element_type=jnp.float32).reshape(
        seq_count, head_count, key_size
    )
    raw_key = jnp.dot(normal_in, w_key, preferred_element_type=jnp.float32).reshape(
        seq_count, head_count, key_size
    )
    raw_value = jnp.dot(normal_in, w_value, preferred_element_type=jnp.float32).reshape(
        seq_count, head_count, value_size
    )
    queries = (rotate(raw_query, lengths) * key_size ** (-0.5)).astype(jnp.bfloat16)
    new_keys = rotate(raw_key, lengths).astype(jnp.bfloat16)
    new_values = raw_value.astype(jnp.bfloat16)
    filled = lengths % block_size
    decay_rate = log_decay(head_count)
    places = jnp.arange(block_size, dtype=jnp.int32)
    distance = jnp.maximum(filled[:, None] - places[None, :], 0).astype(jnp.float32)
    live_mask = places[None, :] < filled[:, None]
    head_rows = -(-head_count // 16) * 16
    row_rate = jnp.concatenate([decay_rate, jnp.zeros((head_rows - head_count,), jnp.float32)])
    decay = jnp.where(
        live_mask[:, None, :], jnp.exp(distance[:, None, :] * row_rate[None, :, None]), 0.0
    )
    same_head = jnp.arange(head_rows)[:, None] == jnp.arange(head_count)[None, :]
    spread = jnp.where(same_head[None, :, :, None], queries[:, None], 0).reshape(
        seq_count, head_rows, head_count * key_size
    )
    carry_scale = jnp.exp((filled.astype(jnp.float32)[:, None] + 1.0) * decay_rate[None, :])
    scaled = queries.astype(jnp.float32) * carry_scale[:, :, None]
    columns = jnp.swapaxes(scaled, 1, 2)
    own_weight = jnp.sum(
        queries.astype(jnp.float32) * new_keys.astype(jnp.float32), axis=-1
    ).astype(jnp.bfloat16)
    inside = read_blocks(spread, columns, decay, cache_keys, cache_values, carry_state)
    inside = inside.reshape(seq_count, head_count, value_size)
    inside = inside + own_weight.astype(jnp.float32)[:, :, None] * new_values.astype(jnp.float32)
    headed = (
        normed(inside).astype(jnp.bfloat16).reshape(seq_count, head_count * value_size)
    )
    mixer_out = jnp.dot(headed, w_out, preferred_element_type=jnp.float32)
    residual = widened + normed(mixer_out)
    return (
        residual,
        new_keys.reshape(seq_count, head_count * key_size),
        new_values.reshape(seq_count, head_count * value_size),
    )


def silu(v):
    return v / (1.0 + jnp.exp(-v))


def channel_mixer(
    dims,
    width,
    expert_count,
    block_ref,
    residual_ref,
    mix_ref,
    eg_hbm,
    eu_hbm,
    ed_hbm,
    dg_hbm,
    du_hbm,
    dd_hbm,
    sg_hbm,
    su_hbm,
    sd_hbm,
    out_ref,
    eg,
    eu,
    ed,
    dg,
    du,
    dd,
    sg,
    su,
    sd,
    gathered,
    partial,
    in_core,
    sum_core,
    in2a,
    in2b,
    sum2a,
    sum2b,
    in3a,
    in3b,
    sum3,
    in4,
    total,
    w_sem,
    own_sem,
    gz_s,
    gz_r,
    g2a_s,
    g2a_r,
    g2b_s,
    g2b_r,
    g3a_s,
    g3a_r,
    g3b_s,
    g3b_r,
    g4_s,
    g4_r,
    r1_s,
    r1_r,
    r2a_s,
    r2a_r,
    r2b_s,
    r2b_r,
    r3a_s,
    r3a_r,
    r3b_s,
    r3b_r,
    r4_s,
    r4_r,
):
    zs, ys, xs = dims
    half = width // 2
    me = lax.axis_index("ep")
    core = lax.rem(me, 2)
    x = lax.rem(me // 2, xs)
    y = lax.rem(me // (2 * xs), ys)
    z = me // (2 * xs * ys)
    other = 1 - core

    def turn(at, by, size):
        return lax.rem(at + by + size, size)

    def device(zz, yy, xx, cc):
        return ((zz * ys + yy) * xs + xx) * 2 + cc

    def z_peer(by):
        return device(turn(z, by, zs), y, x, core)

    def y_peer(by):
        return device(z, turn(y, by, ys), x, core)

    def x_peer(by):
        return device(z, y, turn(x, by, xs), core)

    mate = device(z, y, x, other)
    peers = (
        [z_peer(p) for p in range(1, zs)]
        + [y_peer(p) for p in range(1, ys)]
        + [x_peer(p) for p in range(1, xs)]
        + [mate]
    )

    loads = []
    for at, (a, b) in enumerate(
        [
            (sg_hbm, sg),
            (su_hbm, su),
            (sd_hbm, sd),
            (eg_hbm.at[0], eg),
            (eu_hbm.at[0], eu),
            (ed_hbm.at[0], ed),
            (dg_hbm, dg),
            (du_hbm, du),
            (dd_hbm, dd),
        ]
    ):
        load = pltpu.make_async_copy(a, b, w_sem.at[at])
        load.start()
        loads.append(load)
    own = pltpu.make_async_copy(block_ref, gathered.at[z, y, x, core], own_sem)
    own.start()

    barrier = pltpu.get_barrier_semaphore()
    for peer in peers:
        pl.semaphore_signal(
            barrier, inc=1, device_id=(peer,), device_id_type=pl.DeviceIdType.MESH
        )
    pl.semaphore_wait(barrier, len(peers))

    started = []

    def send(source, target, send_sem, recv_sem, peer):
        copy = pltpu.make_async_remote_copy(
            src_ref=source,
            dst_ref=target,
            send_sem=send_sem,
            recv_sem=recv_sem,
            device_id=(peer,),
            device_id_type=pl.DeviceIdType.MESH,
        )
        copy.start()
        started.append(copy)
        return copy

    own.wait()
    for_z, for2, for3, for4 = {}, {}, {}, {}
    for o in range(1, zs):
        mine = gathered.at[z, y, x, core]
        for_z[o] = send(mine, mine, gz_s.at[o - 1], gz_r.at[o - 1], z_peer(o))

    def spread2(o):
        at = turn(z, -o, zs)
        if o:
            for_z[o].wait_recv()
        a = gathered.at[at, y, x, core, :, pl.ds(0, half)]
        b = gathered.at[at, y, x, core, :, pl.ds(half, gathered.shape[-1] - half)]
        for2[o] = [
            send(a, a, g2a_s.at[o, p - 1], g2a_r.at[o, p - 1], y_peer(p)) for p in range(1, ys)
        ] + [send(b, b, g2b_s.at[o, p - 1], g2b_r.at[o, p - 1], x_peer(p)) for p in range(1, xs)]

    def spread3(o):
        at = turn(z, -o, zs)
        for copy in for2[o]:
            copy.wait_recv()
        a = gathered.at[at, :, x, core, :, pl.ds(0, half)]
        b = gathered.at[at, y, :, core, :, pl.ds(half, gathered.shape[-1] - half)]
        for3[o] = [
            send(a, a, g3a_s.at[o, p - 1], g3a_r.at[o, p - 1], x_peer(p)) for p in range(1, xs)
        ] + [send(b, b, g3b_s.at[o, p - 1], g3b_r.at[o, p - 1], y_peer(p)) for p in range(1, ys)]

    def spread4(o):
        at = turn(z, -o, zs)
        for copy in for3[o]:
            copy.wait_recv()
        a = gathered.at[at, :, :, core]
        for4[o] = send(a, a, g4_s.at[o], g4_r.at[o], mate)

    to1, to2, to3, to4 = {}, {}, {}, {}
    gate = 1.0 / (1.0 + jnp.exp(-mix_ref[...]))

    def branches(o):
        at = turn(z, -o, zs)
        if o == 0:
            for load in loads[3:]:
                load.wait()
        for4[o].wait_recv()
        rows = ys * xs * 2 * gathered.shape[4]
        block = gathered[at].reshape(rows, gathered.shape[-1])
        inputs = block[:, :width]
        extra = block[:, width:].astype(f32)
        lane = lax.broadcasted_iota(jnp.int32, extra.shape, 1)
        chosen = (lane == me) | (lane == me + expert_count)
        weight = jnp.sum(jnp.where(chosen, extra, 0.0), axis=1, keepdims=True)
        hidden = (silu(mm(inputs, eg[...])) * mm(inputs, eu[...])).astype(bf16)
        dense = (silu(mm_t(inputs, dg[...])) * mm_t(inputs, du[...])).astype(bf16)
        terms = weight * mm(hidden, ed[...]) + gate * mm(dense, dd[...])
        partial[at] = terms.astype(bf16).reshape(partial.shape[1:])
        to1[o] = send(
            partial.at[at, :, :, other], in_core.at[o], r1_s.at[o], r1_r.at[o], mate
        )

    def reduce2(o):
        at = turn(z, -o, zs)
        to1[o].wait_recv()
        sum_core[o] = (partial[at, :, :, core].astype(f32) + in_core[o].astype(f32)).astype(bf16)
        to2[o] = [
            send(
                sum_core.at[o, :, turn(x, p, xs), :, pl.ds(0, half)],
                in2a.at[o, p - 1],
                r2a_s.at[o, p - 1],
                r2a_r.at[o, p - 1],
                x_peer(p),
            )
            for p in range(1, xs)
        ] + [
            send(
                sum_core.at[o, turn(y, p, ys), :, :, pl.ds(half, width - half)],
                in2b.at[o, p - 1],
                r2b_s.at[o, p - 1],
                r2b_r.at[o, p - 1],
                y_peer(p),
            )
            for p in range(1, ys)
        ]

    def reduce3(o):
        for copy in to2[o]:
            copy.wait_recv()
        a = sum_core[o, :, x, :, 0:half].astype(f32)
        for p in range(1, xs):
            a = a + in2a[o, p - 1].astype(f32)
        sum2a[o] = a.astype(bf16)
        b = sum_core[o, y, :, :, half:width].astype(f32)
        for p in range(1, ys):
            b = b + in2b[o, p - 1].astype(f32)
        sum2b[o] = b.astype(bf16)
        to3[o] = [
            send(
                sum2a.at[o, turn(y, p, ys)],
                in3a.at[o, p - 1],
                r3a_s.at[o, p - 1],
                r3a_r.at[o, p - 1],
                y_peer(p),
            )
            for p in range(1, ys)
        ] + [
            send(
                sum2b.at[o, turn(x, p, xs)],
                in3b.at[o, p - 1],
                r3b_s.at[o, p - 1],
                r3b_r.at[o, p - 1],
                x_peer(p),
            )
            for p in range(1, xs)
        ]

    def reduce4(o):
        for copy in to3[o]:
            copy.wait_recv()
        a = sum2a[o, y].astype(f32)
        for p in range(1, ys):
            a = a + in3a[o, p - 1].astype(f32)
        b = sum2b[o, x].astype(f32)
        for p in range(1, xs):
            b = b + in3b[o, p - 1].astype(f32)
        if o == 0:
            total[:, 0:half] = total[:, 0:half] + a
            total[:, half:width] = total[:, half:width] + b
        else:
            sum3[o - 1, :, 0:half] = a.astype(bf16)
            sum3[o - 1, :, half:width] = b.astype(bf16)
            to4[o] = send(
                sum3.at[o - 1], in4.at[o - 1], r4_s.at[o - 1], r4_r.at[o - 1], z_peer(-o)
            )

    def shared():
        for load in loads[:3]:
            load.wait()
        inputs = block_ref[:, :width]
        hidden = (silu(mm(inputs, sg[...])) * mm(inputs, su[...])).astype(bf16)
        total[...] = mm(hidden, sd[...])

    stages = [spread2, spread3, spread4, branches, reduce2, reduce3, reduce4]
    for step in range(zs + len(stages) - 1):
        for at, stage in enumerate(stages):
            if 0 <= step - at < zs:
                stage(step - at)
        if step == 0:
            shared()

    combined = total[...]
    for o in range(1, zs):
        to4[o].wait_recv()
        combined = combined + in4[o - 1].astype(f32)
    scale = lax.rsqrt(jnp.mean(combined * combined, axis=-1, keepdims=True) + eps)
    out_ref[...] = (residual_ref[...] + combined * scale).astype(bf16)
    for copy in started:
        copy.wait_send()


def mixed_channels(block, residual, dense_mix, weights, expert_count, device_count):
    seq_count, width = residual.shape
    wide = block.shape[1]
    zs, ys, xs = slice_dims(device_count)
    half = width // 2
    rest = width - half
    y1, x1, z1 = max(ys - 1, 1), max(xs - 1, 1), max(zs - 1, 1)
    held = [pltpu.VMEM(w.shape[-2:], bf16) for w in weights]
    dma = pltpu.SemaphoreType.DMA
    buffers = [
        pltpu.VMEM((zs, ys, xs, 2, seq_count, wide), bf16),
        pltpu.VMEM((zs, ys, xs, 2, seq_count, width), bf16),
        pltpu.VMEM((zs, ys, xs, seq_count, width), bf16),
        pltpu.VMEM((zs, ys, xs, seq_count, width), bf16),
        pltpu.VMEM((zs, x1, ys, seq_count, half), bf16),
        pltpu.VMEM((zs, y1, xs, seq_count, rest), bf16),
        pltpu.VMEM((zs, ys, seq_count, half), bf16),
        pltpu.VMEM((zs, xs, seq_count, rest), bf16),
        pltpu.VMEM((zs, y1, seq_count, half), bf16),
        pltpu.VMEM((zs, x1, seq_count, rest), bf16),
        pltpu.VMEM((z1, seq_count, width), bf16),
        pltpu.VMEM((z1, seq_count, width), bf16),
        pltpu.VMEM((seq_count, width), f32),
    ]
    sems = [dma((len(weights),)), dma]
    for shape in [
        (z1,),
        (zs, y1),
        (zs, x1),
        (zs, x1),
        (zs, y1),
        (zs,),
        (zs,),
        (zs, x1),
        (zs, y1),
        (zs, y1),
        (zs, x1),
        (z1,),
    ]:
        sems += [dma(shape), dma(shape)]
    vmem = pl.BlockSpec(memory_space=pltpu.VMEM)
    return pl.pallas_call(
        functools.partial(channel_mixer, (zs, ys, xs), width, expert_count),
        out_shape=jax.ShapeDtypeStruct((seq_count, width), bf16),
        in_specs=[vmem] * 3 + [pl.BlockSpec(memory_space=pl.ANY)] * len(weights),
        out_specs=vmem,
        scratch_shapes=held + buffers + sems,
        compiler_params=pltpu.CompilerParams(
            collective_id=0, has_side_effects=True, vmem_limit_bytes=56 * 1024 * 1024
        ),
    )(block, residual, dense_mix.reshape(1, width), *weights)


def per_device(
    tokens,
    lengths,
    cache_keys,
    cache_values,
    retention_state,
    mix_gain,
    query_weight,
    key_weight,
    value_weight,
    out_weight,
    ffn_gain,
    routes,
    route_scores,
    expert_gate,
    expert_up,
    expert_down,
    shared_gate,
    shared_up,
    shared_down,
    dense_gate,
    dense_up,
    dense_down,
    dense_mix,
):
    residual, new_keys, new_values = retain(
        tokens,
        lengths,
        mix_gain,
        query_weight,
        key_weight,
        value_weight,
        out_weight,
        cache_keys,
        cache_values,
        retention_state,
    )
    normal_ffn = (normed(residual) * ffn_gain).astype(jnp.bfloat16)
    device_count = lax.axis_size("ep")
    expert_count = device_count * expert_gate.shape[0]
    route_weight = route_scores / jnp.sum(route_scores, axis=-1, keepdims=True) * route_scale
    named = routes[:, :, None] == jnp.arange(expert_count, dtype=jnp.int32)[None, None, :]
    by_expert = jnp.sum(jnp.where(named, route_weight[:, :, None], 0.0), axis=1)
    upper = lax.reduce_precision(by_expert, 8, 7)
    pad = -(2 * expert_count) % 128
    block = jnp.concatenate(
        [
            normal_ffn,
            upper.astype(bf16),
            (by_expert - upper).astype(bf16),
            jnp.zeros((routes.shape[0], pad), bf16),
        ],
        axis=1,
    )
    weights = (
        expert_gate,
        expert_up,
        expert_down,
        dense_gate,
        dense_up,
        dense_down,
        shared_gate,
        shared_up,
        shared_down,
    )
    layer_out = mixed_channels(block, residual, dense_mix, weights, expert_count, device_count)
    return (layer_out, new_keys, new_values)


def solution(mesh):
    in_specs = (
        P("ep", None),
        P("ep"),
        P("ep", None, None),
        P("ep", None, None),
        P("ep", None, None, None),
        P(),
        P(),
        P(),
        P(),
        P(),
        P(),
        P("ep", None),
        P("ep", None),
        P("ep", None, None),
        P("ep", None, None),
        P("ep", None, None),
        P(),
        P(),
        P(),
        P("ep", None),
        P("ep", None),
        P("ep", None),
        P(),
    )
    out_specs = (P("ep", None), P("ep", None), P("ep", None))
    return jax.shard_map(
        per_device, mesh=mesh, in_specs=in_specs, out_specs=out_specs, check_vma=False
    )
```
